32 devices in a mesh: sp: 4 (over z), fs: 4 (over y, x), tp: 2 (over core).
Axes of the slice: x: 2, y: 2, z: 4, core: 2. Of those that a mesh axis runs over, the one named last changes fastest.
Arguments:
- tokens: bfloat16 [4, 1024, 2048], P('fs', 'sp'), may hold values from -6 to 6
- mix_gain: float32 [2048], replicated, may hold values from 0.1 to 1.9
- query_down: bfloat16 [2048, 768], P('fs', 'tp'), may hold values from -0.125 to 0.125
- memory_down: bfloat16 [2048, 512], P('fs', 'tp'), may hold values from -0.125 to 0.125
- rope_weight: bfloat16 [2048, 32], replicated, may hold values from -0.125 to 0.125
- query_up: bfloat16 [768, 1536], P('fs', 'tp'), may hold values from -0.21875 to 0.21875
- key_up: bfloat16 [512, 1024], P('fs', 'tp'), may hold values from -0.25 to 0.25
- value_up: bfloat16 [512, 1024], P('fs', 'tp'), may hold values from -0.25 to 0.25
- latent_gain: float32 [768], replicated, may hold values from 0.1 to 1.9
- memory_gain: float32 [512], replicated, may hold values from 0.1 to 1.9
- query_gain: float32 [96], replicated, may hold values from 1 to 16
- key_gain: float32 [96], replicated, may hold values from 0.1 to 1.9
- conv_value: bfloat16 [2048, 1024], P('fs', 'tp'), may hold values from -1 to 1
- conv_gate: bfloat16 [2048, 1024], P('fs', 'tp'), may hold values from -0.125 to 0.125
- conv_kernel: bfloat16 [31, 1024], P(None, 'tp'), may hold values from -50 to 50
- channel_gain: float32 [1024], P('tp'), may hold values from 0.1 to 1.9
- channel_shift: float32 [1024], P('tp'), may hold values from -3 to 3
- heads_out: bfloat16 [1024, 2048], P('tp', 'fs'), may hold values from -0.75 to 0.75
- conv_out: bfloat16 [1024, 2048], P('tp', 'fs'), may hold values from -0.1875 to 0.1875
Outputs:
- mixed: bfloat16 [4, 1024, 2048], P('fs', 'sp')
The draws below stay inside these ranges and needn't reach their ends.
All inputs are finite; a program needn't handle non-finite values.
Results may differ from the reference program's by a relative error of at most 0.015.
The reference program's roundings to bfloat16 on the way count: a program that leaves them out, or rounds other values in their place, can miss the bound.
Values may be sent and summed in bfloat16 or wider, within the bound.
A program may use at most 64 MiB of HBM per device.

```python
import math
import jax
import jax.numpy as jnp
from jax import lax

D = 2048
HEADS = 16
QK_NOPE = 64
QK_ROPE = 32
V_DIM = 64
Q_LAT = 768
KV_LAT = 512
CONV_W = 1024
CONV_K = 31
SEG = 64
TOK_DEV = 256
QK_DIM = 96
SEQ = 1024
SEQS = 4
N_TP = 2


def draw_query_gain(key, part):
    gain_key = jax.random.fold_in(key, 11)
    return jnp.exp(jax.random.uniform(gain_key, (QK_DIM,), jnp.float32, 0.0, math.log(3.0)))


def draw_conv_value(key, part):
    noise_key, common_key, level_key = jax.random.split(jax.random.fold_in(key, 23), 3)
    noise = jnp.clip(jax.random.normal(noise_key, (D, CONV_W), jnp.float32), -5.0, 5.0)
    common = jnp.clip(jax.random.normal(common_key, (D,), jnp.float32), -5.0, 5.0)
    level = jax.random.uniform(level_key, (CONV_W,), jnp.float32, 0.5, 1.5)
    strength = 0.7
    return ((noise + strength * common[:, None] * level[None, :]) / math.sqrt(D)).astype(jnp.bfloat16)


def draw_conv_kernel(key, part):
    noise_key, scale_key = jax.random.split(jax.random.fold_in(key, 7))
    channel_pos = jnp.arange(CONV_W, dtype=jnp.float32) / CONV_W
    roughness = jnp.exp(jax.random.uniform(scale_key, (CONV_W,), jnp.float32, -0.7, 0.7))
    channel_scale = 10.0 ** channel_pos * roughness
    tap_draw = jnp.clip(jax.random.normal(noise_key, (CONV_K, CONV_W), jnp.float32), -5.0, 5.0)
    return ((tap_draw + 1.0) * channel_scale[None, :] / math.sqrt(CONV_K)).astype(jnp.bfloat16)


def steps_of(own_key, shape, cuts, least, top_value):
    level, own = 1.0, jax.random.fold_in(own_key, 6)
    for axis_at, shards_of in cuts:
        heights = jnp.exp(jax.random.uniform(jax.random.fold_in(own, axis_at), (shards_of,), jnp.float32, least / len(cuts), top_value / len(cuts)))
        level = level * jnp.repeat(heights, shape[axis_at] // shards_of).reshape([-1 if axis == axis_at else 1 for axis in range(len(shape))])
    return level


def gaussian(own_key, extent, width, reach, cuts=(), kind=jnp.bfloat16):
    factor_of = steps_of(own_key, extent, cuts, -0.22, 0.18) if cuts else 1.0
    drawn = jax.random.normal(own_key, extent, jnp.float32) * width * factor_of
    return jnp.minimum(jnp.maximum(drawn, -reach), reach).astype(kind)


def setup_inputs(seed: int = 0) -> dict:
    arg_keys = jax.random.split(jax.random.key(seed), 20)
    return {
        "tokens": gaussian(arg_keys[0], (SEQS, SEQ, D), 1.0, 6.0, ((0, 4), (1, 4))),
        "mix_gain": jnp.clip(1.0 + 0.18 * jax.random.normal(arg_keys[1], (D,), jnp.float32), 0.1, 1.9),
        "query_down": gaussian(arg_keys[2], (D, Q_LAT), D ** -0.5, 0.125, ((0, 4), (1, 2))),
        "memory_down": gaussian(arg_keys[3], (D, KV_LAT), D ** -0.5, 0.125, ((0, 4), (1, 2))),
        "rope_weight": gaussian(arg_keys[4], (D, QK_ROPE), D ** -0.5, 0.125),
        "query_up": gaussian(arg_keys[5], (Q_LAT, HEADS * QK_DIM), Q_LAT ** -0.5, 0.21875, ((0, 4), (1, 2))),
        "key_up": gaussian(arg_keys[6], (KV_LAT, HEADS * QK_NOPE), KV_LAT ** -0.5, 0.25, ((0, 4), (1, 2))),
        "value_up": gaussian(arg_keys[7], (KV_LAT, HEADS * V_DIM), KV_LAT ** -0.5, 0.25, ((0, 4), (1, 2))),
        "latent_gain": jnp.clip(1.0 + 0.18 * jax.random.normal(arg_keys[8], (Q_LAT,), jnp.float32), 0.1, 1.9),
        "memory_gain": jnp.clip(1.0 + 0.18 * jax.random.normal(arg_keys[9], (KV_LAT,), jnp.float32), 0.1, 1.9),
        "query_gain": draw_query_gain(jax.random.fold_in(arg_keys[19], 71), 0),
        "key_gain": jnp.clip(1.0 + 0.18 * jax.random.normal(arg_keys[11], (QK_DIM,), jnp.float32), 0.1, 1.9),
        "conv_value": draw_conv_value(jax.random.fold_in(arg_keys[19], 71), 0),
        "conv_gate": gaussian(arg_keys[13], (D, CONV_W), D ** -0.5, 0.125, ((0, 4), (1, 2))),
        "conv_kernel": draw_conv_kernel(jax.random.fold_in(arg_keys[19], 71), 0),
        "channel_gain": jnp.clip(1.0 + 0.18 * jax.random.normal(arg_keys[15], (CONV_W,), jnp.float32), 0.1, 1.9),
        "channel_shift": gaussian(arg_keys[16], (CONV_W,), 0.5, 3.0, ((0, 2),), jnp.float32),
        "heads_out": gaussian(arg_keys[17], (HEADS * V_DIM, D), V_DIM ** -0.5, 0.75, ((0, 2), (1, 4))),
        "conv_out": gaussian(arg_keys[18], (CONV_W, D), CONV_W ** -0.5, 0.1875, ((0, 2), (1, 4))),
    }


epsilon = 1e-06
rope_base = 10000.0
masked_score = -1e+30

def norm_rows(matrix, scale_vector):
    return matrix * lax.rsqrt(lax.optimization_barrier(jnp.mean(matrix * matrix, axis=-1, keepdims=True)) + epsilon) * scale_vector.astype(jnp.float32)

def rope_tables(positions):
    inverse_freq = 1.0 / rope_base ** (jnp.arange(0, QK_ROPE, 2, dtype=jnp.float32) / QK_ROPE)
    angles = positions.astype(jnp.float32)[:, None] * inverse_freq[None, :]
    return (jnp.cos(angles)[:, None, :], jnp.sin(angles)[:, None, :])

def rotate(matrix, cosine_table, sine_table):
    half_width = matrix.shape[-1] // 2
    front_half = matrix[..., :half_width]
    back_half = matrix[..., half_width:]
    return jnp.concatenate([front_half * cosine_table - back_half * sine_table, front_half * sine_table + back_half * cosine_table], axis=-1)

def heads_query(latent, weight, scale_vector, cosine_table, sine_table):
    row_count = latent.shape[0]
    projected = jnp.dot(latent, weight, preferred_element_type=jnp.float32)
    projected = norm_rows(projected.reshape(row_count, weight.shape[1] // QK_DIM, QK_DIM), scale_vector)
    turned = rotate(projected[..., QK_NOPE:], cosine_table, sine_table)
    return jnp.concatenate([projected[..., :QK_NOPE], turned], axis=-1).astype(jnp.bfloat16)

def heads_key(latent, rope_rows, weight, scale_vector, cosine_table, sine_table):
    row_count = latent.shape[0]
    head_count = weight.shape[1] // QK_NOPE
    nope_part = jnp.dot(latent, weight, preferred_element_type=jnp.float32).reshape(row_count, head_count, QK_NOPE)
    shared = jnp.broadcast_to(rope_rows.astype(jnp.float32)[:, None, :], (row_count, head_count, QK_ROPE))
    joined = norm_rows(jnp.concatenate([nope_part, shared], axis=-1), scale_vector)
    turned = rotate(joined[..., QK_NOPE:], cosine_table, sine_table)
    return jnp.concatenate([joined[..., :QK_NOPE], turned], axis=-1).astype(jnp.bfloat16)

def depthwise(extended, kernel, row_count):

    def add_tap(tap_index, running):
        window = lax.dynamic_slice_in_dim(extended, tap_index.astype(jnp.int32), row_count, 0).astype(jnp.float32)
        weight_row = lax.dynamic_slice_in_dim(kernel, tap_index.astype(jnp.int32), 1, 0).astype(jnp.float32)
        return running + window * weight_row
    return lax.fori_loop(0, kernel.shape[0], add_tap, jnp.zeros((row_count, kernel.shape[1]), jnp.float32))

def attention_block(queries, key_rows, value_rows, query_pos):
    key_pos = jnp.arange(key_rows.shape[0], dtype=jnp.int32)
    scores = jnp.einsum('qhd,khd->qhk', queries.astype(jnp.float32), key_rows.astype(jnp.float32)) * QK_DIM ** (-0.5)
    allowed = ((key_pos // SEG)[None, :] <= (query_pos // SEG)[:, None])[:, None, :]
    scores = jnp.where(allowed, scores, masked_score)
    row_max = lax.optimization_barrier(jnp.max(scores, axis=2, keepdims=True))
    weights = jnp.where(allowed, jnp.exp(scores - row_max), 0.0)
    row_total = lax.optimization_barrier(jnp.sum(weights, axis=2))
    rounded = weights.astype(jnp.bfloat16)
    summed = jnp.einsum('qhk,khd->qhd', rounded.astype(jnp.float32), value_rows.astype(jnp.float32))
    return (summed / row_total[:, :, None]).astype(jnp.bfloat16)

def one_sequence(tokens, mix_gain, query_down, memory_down, rope_weight, query_up, key_up, value_up, latent_gain, memory_gain, query_gain, key_gain, conv_value, conv_gate, conv_kernel, channel_gain, channel_shift, heads_out, conv_out):
    normed = norm_rows(tokens.astype(jnp.float32), mix_gain).astype(jnp.bfloat16)
    latent_query = jnp.dot(normed, query_down, preferred_element_type=jnp.float32).astype(jnp.bfloat16)
    latent_memory = jnp.dot(normed, memory_down, preferred_element_type=jnp.float32).astype(jnp.bfloat16)
    rope_rows = jnp.dot(normed, rope_weight, preferred_element_type=jnp.float32).astype(jnp.bfloat16)
    value_part = jnp.dot(normed, conv_value, preferred_element_type=jnp.float32)
    gate_part = jnp.dot(normed, conv_gate, preferred_element_type=jnp.float32)
    gated = (value_part * jax.nn.sigmoid(gate_part)).astype(jnp.bfloat16)
    query_normed = norm_rows(latent_query.astype(jnp.float32), latent_gain).astype(jnp.bfloat16)
    memory_normed = norm_rows(latent_memory.astype(jnp.float32), memory_gain).astype(jnp.bfloat16)
    positions = jnp.arange(SEQ, dtype=jnp.int32)
    cosine_table, sine_table = rope_tables(positions)
    queries = heads_query(query_normed, query_up, query_gain, cosine_table, sine_table)
    key_rows = heads_key(memory_normed, rope_rows, key_up, key_gain, cosine_table, sine_table)
    value_rows = jnp.dot(memory_normed, value_up, preferred_element_type=jnp.float32).astype(jnp.bfloat16).reshape(SEQ, HEADS, V_DIM)
    query_blocks = queries.reshape(SEQ // TOK_DEV, TOK_DEV, HEADS, QK_DIM)
    block_pos = positions.reshape(SEQ // TOK_DEV, TOK_DEV)

    def per_block(pair):
        return attention_block(pair[0], key_rows, value_rows, pair[1])
    attention = lax.map(per_block, (query_blocks, block_pos)).reshape(SEQ, HEADS * V_DIM)
    extended = jnp.concatenate([jnp.zeros((CONV_K - 1, CONV_W), jnp.bfloat16), gated], axis=0)
    conv_sum = depthwise(extended, conv_kernel, SEQ)
    row_mean = lax.optimization_barrier(jnp.mean(conv_sum, axis=1, keepdims=True))
    centered = conv_sum - row_mean
    spread = lax.optimization_barrier(jnp.mean(centered * centered, axis=1, keepdims=True))
    conv_result = jax.nn.silu(centered * lax.rsqrt(spread + epsilon) * channel_gain.astype(jnp.float32) + channel_shift.astype(jnp.float32)).astype(jnp.bfloat16)
    attn_width = HEADS * V_DIM // N_TP
    conv_width = CONV_W // N_TP
    mixed = jnp.zeros((SEQ, D), jnp.float32)
    for group_index in range(N_TP):
        head_cols = slice(group_index * attn_width, (group_index + 1) * attn_width)
        conv_cols = slice(group_index * conv_width, (group_index + 1) * conv_width)
        partial_sum = jnp.dot(attention[:, head_cols], heads_out[head_cols], preferred_element_type=jnp.float32)
        partial_sum = partial_sum + jnp.dot(conv_result[:, conv_cols], conv_out[conv_cols], preferred_element_type=jnp.float32)
        mixed = mixed + lax.optimization_barrier(partial_sum.astype(jnp.bfloat16)).astype(jnp.float32)
    return mixed.astype(jnp.bfloat16)

def reference(tokens, mix_gain, query_down, memory_down, rope_weight, query_up, key_up, value_up, latent_gain, memory_gain, query_gain, key_gain, conv_value, conv_gate, conv_kernel, channel_gain, channel_shift, heads_out, conv_out):

    def per_sequence(sequence):
        return one_sequence(sequence, mix_gain, query_down, memory_down, rope_weight, query_up, key_up, value_up, latent_gain, memory_gain, query_gain, key_gain, conv_value, conv_gate, conv_kernel, channel_gain, channel_shift, heads_out, conv_out)
    return lax.map(per_sequence, tokens)
```

```python
import functools

import jax
import jax.numpy as jnp
from jax import lax
from jax.experimental import pallas as pl
from jax.experimental.pallas import tpu as pltpu
from jax.sharding import PartitionSpec as P

MESH_ID = pl.DeviceIdType.MESH

QK_NOPE = 64
QK_ROPE = 32
V_DIM = 64
CONV_W = 1024
SEG = 64
QK_DIM = 96


epsilon = 1e-06
rope_base = 10000.0
masked_score = -1e30


def norm_rows(matrix, scale_vector):
    return (
        matrix
        * lax.rsqrt(jnp.mean(matrix * matrix, axis=-1, keepdims=True) + epsilon)
        * scale_vector
    )


def rope_tables(positions):
    inverse_freq = 1.0 / rope_base ** (jnp.arange(0, QK_ROPE, 2, dtype=jnp.float32) / QK_ROPE)
    angles = positions.astype(jnp.float32)[:, None] * inverse_freq[None, :]
    return (jnp.cos(angles)[:, None, :], jnp.sin(angles)[:, None, :])


def rotate(matrix, cosine_table, sine_table):
    half_width = matrix.shape[-1] // 2
    front_half = matrix[..., :half_width]
    back_half = matrix[..., half_width:]
    return jnp.concatenate(
        [
            front_half * cosine_table - back_half * sine_table,
            front_half * sine_table + back_half * cosine_table,
        ],
        axis=-1,
    )


def heads_query(latent, weight, scale_vector, cosine_table, sine_table):
    row_count = latent.shape[0]
    projected = jnp.dot(latent, weight, preferred_element_type=jnp.float32)
    projected = norm_rows(
        projected.reshape(row_count, weight.shape[1] // QK_DIM, QK_DIM), scale_vector
    )
    turned = rotate(projected[..., QK_NOPE:], cosine_table, sine_table)
    return jnp.concatenate([projected[..., :QK_NOPE], turned], axis=-1).astype(jnp.bfloat16)


def heads_key(latent, rope_rows, weight, scale_vector, cosine_table, sine_table):
    row_count = latent.shape[0]
    head_count = weight.shape[1] // QK_NOPE
    nope_part = jnp.dot(latent, weight, preferred_element_type=jnp.float32).reshape(
        row_count, head_count, QK_NOPE
    )
    shared = jnp.broadcast_to(
        rope_rows.astype(jnp.float32)[:, None, :], (row_count, head_count, QK_ROPE)
    )
    joined = norm_rows(jnp.concatenate([nope_part, shared], axis=-1), scale_vector)
    turned = rotate(joined[..., QK_NOPE:], cosine_table, sine_table)
    return jnp.concatenate([joined[..., :QK_NOPE], turned], axis=-1).astype(jnp.bfloat16)


RIM = 32


def relayed_rows(rows, paired):
    return (rows * 3 // 8) // 16 * 16 if paired else 0


def gather_kernel(
    sizes,
    x_ref, gain_ref, rope_ref, taps_ref,
    qd, md, cv, cg, qu, ku, vu, ho, co,
    lq_ref, lm_ref, rr_ref, sum_ref, qu_all, ku_all, vu_all, ho_all, co_all,
    qd_all, md_all, cv_all, cg_all, normed, acc_q, acc_v, acc_g, ext, tail, rim,
    send_a, recv_a, send_z, recv_z, local_sem, rim_sem,
):
    n_fs, n_sp = sizes
    paired = n_sp % 2 == 0
    f = lax.axis_index("fs")
    s = lax.axis_index("sp")
    parity = lax.rem(s, 2)
    partner = s + 1 - 2 * parity

    barrier = pltpu.get_barrier_semaphore()
    for k in range(1, n_fs):
        pl.semaphore_signal(
            barrier, inc=1, device_id={"fs": lax.rem(f + k, n_fs)}, device_id_type=MESH_ID
        )

    beside = sorted({1 % n_sp, (n_sp - 1) % n_sp} - {0})
    for step in beside:
        pl.semaphore_signal(
            barrier, inc=1, device_id={"sp": lax.rem(s + step, n_sp)}, device_id_type=MESH_ID
        )
    pl.semaphore_wait(barrier, n_fs - 1 + len(beside))

    jobs = [
        (qd, qd_all, 0), (md, md_all, 0), (cv, cv_all, 0), (cg, cg_all, 0),
        (qu, qu_all, 0), (ku, ku_all, 0), (vu, vu_all, 0), (ho, ho_all, 1), (co, co_all, 1),
    ]

    def place(whole, shard, dim, owner, start, count):
        rows, cols = shard.shape
        if dim == 0:
            return whole.at[pl.ds(pl.multiple_of(owner * rows + start, 16), count), :]
        return whole.at[
            pl.ds(pl.multiple_of(start, 16), count),
            pl.ds(pl.multiple_of(owner * cols, 128), cols),
        ]

    first, relay, own = [], [], []
    for a, (shard, whole, dim) in enumerate(jobs):
        rows = shard.shape[0]
        less = relayed_rows(rows, paired)
        start = parity * less
        for k in range(1, n_fs):
            copy = pltpu.make_async_remote_copy(
                src_ref=shard.at[pl.ds(pl.multiple_of(start, 16), rows - less), :],
                dst_ref=place(whole, shard, dim, f, start, rows - less),
                send_sem=send_a.at[a, k - 1],
                recv_sem=recv_a.at[a, k - 1],
                device_id={"fs": lax.rem(f + k, n_fs)},
                device_id_type=MESH_ID,
            )
            copy.start()
            first.append(copy)
            if less:
                lack = parity * (rows - less)
                owner = lax.rem(f + n_fs - k, n_fs)
                relay.append(pltpu.make_async_remote_copy(
                    src_ref=place(whole, shard, dim, owner, lack, less),
                    dst_ref=place(whole, shard, dim, owner, lack, less),
                    send_sem=send_z.at[a, k - 1],
                    recv_sem=recv_z.at[a, k - 1],
                    device_id={"sp": partner},
                    device_id_type=MESH_ID,
                ))
        mine = pltpu.make_async_copy(
            shard, place(whole, shard, dim, f, 0, rows), local_sem.at[a]
        )
        mine.start()
        own.append(mine)

    rows = x_ref.shape[0]
    part = 32

    @pl.loop(0, rows // part)
    def _(i):
        at = pl.ds(pl.multiple_of(i * part, part), part)
        x = x_ref[at, :].astype(jnp.float32)
        scale = lax.rsqrt(jnp.mean(x * x, axis=-1, keepdims=True) + epsilon)
        normed[at, :] = (x * scale * gain_ref[...]).astype(jnp.bfloat16)

    per = n_fs - 1

    def pass_on(a):
        for k in range(per):
            first[a * per + k].wait_recv()
            if paired:
                relay[a * per + k].start()

    def complete(a):
        own[a].wait()
        if paired:
            for k in range(per):
                relay[a * per + k].wait_recv()

    depth = qd.shape[0]

    def project(weight, acc):
        acc[...] = jnp.zeros_like(acc)

        @pl.loop(0, n_fs)
        def _(i):
            at = pl.ds(pl.multiple_of(i * depth, depth), depth)
            acc[...] += jnp.dot(
                normed[:, at], weight[at, :], preferred_element_type=jnp.float32
            )

    rr_ref[...] = jnp.dot(
        normed[...], rope_ref[...], preferred_element_type=jnp.float32
    ).astype(jnp.bfloat16)
    pass_on(0)
    pass_on(1)
    complete(0)
    project(qd_all, acc_q)
    lq_ref[...] = acc_q[...].astype(jnp.bfloat16)
    pass_on(2)
    complete(1)
    acc_m = acc_q.at[:, pl.ds(0, md.shape[1])]
    project(md_all, acc_m)
    lm_ref[...] = acc_m[...].astype(jnp.bfloat16)
    pass_on(3)
    complete(2)
    project(cv_all, acc_v)
    pass_on(4)
    complete(3)
    project(cg_all, acc_g)
    pass_on(5)

    @pl.loop(0, rows // part)
    def _(i):
        at = pl.ds(pl.multiple_of(i * part, part), part)
        gated = (acc_v[at, :] * jax.nn.sigmoid(acc_g[at, :])).astype(jnp.bfloat16)
        ext[pl.ds(pl.multiple_of(RIM + i * part, part), part), :] = gated.astype(jnp.float32)

    tail[...] = ext[pl.ds(rows, RIM), :].astype(jnp.bfloat16)
    rim_copy = pltpu.make_async_remote_copy(
        src_ref=tail, dst_ref=rim, send_sem=rim_sem.at[0], recv_sem=rim_sem.at[1],
        device_id={"sp": lax.rem(s + 1, n_sp)}, device_id_type=MESH_ID,
    )

    @pl.when(s < n_sp - 1)
    def _():
        rim_copy.start()

    pass_on(6)

    @pl.when(s > 0)
    def _():
        rim_copy.wait_recv()
        ext[pl.ds(0, RIM), :] = rim[...].astype(jnp.float32)

    @pl.when(s == 0)
    def _():
        ext[pl.ds(0, RIM), :] = jnp.zeros((RIM, ext.shape[1]), jnp.float32)

    pass_on(7)
    tap_count = taps_ref.shape[0]
    block = 64

    @pl.loop(0, ext.shape[1] // 128)
    def _(c):
        cols = pl.ds(pl.multiple_of(c * 128, 128), 128)
        taps = taps_ref[:, cols].astype(jnp.float32)
        for r in range(0, rows, block):
            total = jnp.zeros((block, 128), jnp.float32)
            for j in range(tap_count):
                total = total + ext[
                    pl.ds(r + RIM - (tap_count - 1) + j, block), cols
                ] * taps[j : j + 1, :]
            sum_ref[pl.ds(r, block), cols] = total

    pass_on(8)
    for a in range(4, 9):
        complete(a)
    for copy in first + relay:
        copy.wait_send()

    @pl.when(s < n_sp - 1)
    def _():
        rim_copy.wait_send()


def gather_and_project(
    n_fs, n_sp, x, mix_gain, rope_weight, taps, qd, md, cv, cg, qu, ku, vu, ho, co
):
    rows = x.shape[0]
    bf16, f32 = jnp.bfloat16, jnp.float32
    vmem = pl.BlockSpec(memory_space=pltpu.VMEM)
    hbm = pl.BlockSpec(memory_space=pl.ANY)

    def whole(w, dim=0):
        return (w.shape[0] * n_fs, w.shape[1]) if dim == 0 else (w.shape[0], w.shape[1] * n_fs)

    out_shapes = [
        ((rows, qd.shape[1]), bf16), ((rows, md.shape[1]), bf16),
        ((rows, rope_weight.shape[1]), bf16), ((rows, cv.shape[1]), f32),
        (whole(qu), bf16), (whole(ku), bf16), (whole(vu), bf16),
        (whole(ho, 1), bf16), (whole(co, 1), bf16),
    ]
    dma = pltpu.SemaphoreType.DMA
    wide = max(qd.shape[1], md.shape[1])
    return pl.pallas_call(
        functools.partial(gather_kernel, (n_fs, n_sp)),
        out_shape=[jax.ShapeDtypeStruct(*o) for o in out_shapes],
        in_specs=[vmem] * 4 + [hbm] * 9,
        out_specs=[vmem] * 9,
        scratch_shapes=[
            pltpu.VMEM(whole(qd), bf16), pltpu.VMEM(whole(md), bf16),
            pltpu.VMEM(whole(cv), bf16), pltpu.VMEM(whole(cg), bf16),
            pltpu.VMEM(x.shape, bf16), pltpu.VMEM((rows, wide), f32),
            pltpu.VMEM((rows, cv.shape[1]), f32), pltpu.VMEM((rows, cv.shape[1]), f32),
            pltpu.VMEM((rows + RIM, cv.shape[1]), f32),
            pltpu.VMEM((RIM, cv.shape[1]), bf16), pltpu.VMEM((RIM, cv.shape[1]), bf16),
            dma((9, n_fs - 1)), dma((9, n_fs - 1)), dma((9, n_fs - 1)), dma((9, n_fs - 1)),
            dma((9,)), dma((2,)),
        ],
        compiler_params=pltpu.CompilerParams(
            collective_id=0, has_side_effects=True, vmem_limit_bytes=56 * 1024 * 1024
        ),
    )(x, mix_gain[None, :], rope_weight, taps, qd, md, cv, cg, qu, ku, vu, ho, co)


def key_block(key_count):
    block_size = key_count
    while block_size > 2048 and block_size % 2 == 0:
        block_size = block_size // 2
    return block_size


def sum_groups(partial):
    count = lax.axis_size("tp")
    if count != 2:
        return lax.psum(partial, "tp")
    other = lax.ppermute(partial, "tp", [(0, 1), (1, 0)])
    return (partial.astype(jnp.float32) + other.astype(jnp.float32)).astype(jnp.bfloat16)


def local(
    tokens,
    mix_gain,
    query_down,
    memory_down,
    rope_weight,
    query_up,
    key_up,
    value_up,
    latent_gain,
    memory_gain,
    query_gain,
    key_gain,
    conv_value,
    conv_gate,
    conv_kernel,
    channel_gain,
    channel_shift,
    heads_out,
    conv_out,
):
    own_rows = tokens[0]
    (
        latent_query, latent_memory, rope_rows, conv_sum,
        up_query, up_keys, up_values, out_heads, out_conv,
    ) = gather_and_project(
        lax.axis_size("fs"), lax.axis_size("sp"), own_rows, mix_gain, rope_weight, conv_kernel,
        query_down, memory_down, conv_value, conv_gate,
        query_up, key_up, value_up, heads_out, conv_out,
    )
    row_count = own_rows.shape[0]
    whole_query, whole_memory = (
        lax.all_gather(latent_query, "tp", axis=1, tiled=True),
        lax.all_gather(latent_memory, "tp", axis=1, tiled=True),
    )
    query_normed = norm_rows(whole_query.astype(jnp.float32), latent_gain).astype(jnp.bfloat16)
    memory_normed = norm_rows(whole_memory.astype(jnp.float32), memory_gain).astype(jnp.bfloat16)
    positions = lax.axis_index("sp") * row_count + jnp.arange(row_count, dtype=jnp.int32)
    cosine_table, sine_table = rope_tables(positions)
    queries = heads_query(query_normed, up_query, query_gain, cosine_table, sine_table)
    head_count = queries.shape[1]
    query_segment = positions // SEG
    score_scale = QK_DIM ** (-0.5)
    row_sums, row_squares = lax.psum(
        (jnp.sum(conv_sum, axis=1), jnp.sum(conv_sum * conv_sum, axis=1)), "tp"
    )
    row_mean = row_sums / CONV_W
    spread = row_squares / CONV_W - row_mean * row_mean
    centered = conv_sum - row_mean[:, None]
    conv_result = jax.nn.silu(
        centered * lax.rsqrt(spread[:, None] + epsilon) * channel_gain + channel_shift
    ).astype(jnp.bfloat16)

    def attend(state_carry, key_rows, value_rows, key_pos):
        running_max, row_total, weighted = state_carry
        scores = (
            jnp.einsum("qhd,khd->qhk", queries, key_rows, preferred_element_type=jnp.float32)
            * score_scale
        )
        allowed = ((key_pos // SEG)[None, :] <= query_segment[:, None])[:, None, :]
        scores = jnp.where(allowed, scores, masked_score)
        new_max = jnp.maximum(running_max, jnp.max(scores, axis=2))
        weights = jnp.where(allowed, jnp.exp(scores - new_max[:, :, None]), 0.0)
        factor = jnp.exp(running_max - new_max)
        row_total = row_total * factor + jnp.sum(weights, axis=2)
        weighted = weighted * factor[:, :, None] + jnp.einsum(
            "qhk,khd->qhd",
            weights.astype(jnp.bfloat16),
            value_rows,
            preferred_element_type=jnp.float32,
        )
        return (new_max, row_total, weighted)

    initial = (
        jnp.full((row_count, head_count), masked_score, jnp.float32),
        jnp.zeros((row_count, head_count), jnp.float32),
        jnp.zeros((row_count, head_count, V_DIM), jnp.float32),
    )
    memory_piece = lax.all_gather(memory_normed, "sp", axis=0, tiled=True)
    rope_piece = lax.all_gather(rope_rows, "sp", axis=0, tiled=True)

    def block_keys(block_start, block_size):
        memory_block = lax.dynamic_slice_in_dim(memory_piece, block_start, block_size, 0)
        rope_block = lax.dynamic_slice_in_dim(rope_piece, block_start, block_size, 0)
        key_pos = block_start + jnp.arange(block_size, dtype=jnp.int32)
        cosine_keys, sine_keys = rope_tables(key_pos)
        key_rows = heads_key(memory_block, rope_block, up_keys, key_gain, cosine_keys, sine_keys)
        value_rows = (
            jnp.dot(memory_block, up_values, preferred_element_type=jnp.float32)
            .astype(jnp.bfloat16)
            .reshape(block_size, head_count, V_DIM)
        )
        return (key_rows, value_rows, key_pos)

    key_count = memory_piece.shape[0]
    block_size = key_block(key_count)

    def step(block_index, running):
        key_rows, value_rows, key_pos = block_keys(block_index * block_size, block_size)
        return attend(running, key_rows, value_rows, key_pos)

    final_state = lax.fori_loop(0, key_count // block_size, step, initial)
    running_max, row_total, weighted = final_state
    attention = (
        (weighted / row_total[:, :, None])
        .astype(jnp.bfloat16)
        .reshape(row_count, head_count * V_DIM)
    )
    mixer_rows = jnp.concatenate([attention, conv_result], axis=1)
    out_weight = jnp.concatenate([out_heads, out_conv], axis=0)
    partial_sum = jnp.dot(mixer_rows, out_weight, preferred_element_type=jnp.float32)
    mixed = sum_groups(partial_sum.astype(jnp.bfloat16))
    return mixed[None]


def solution(mesh):
    in_specs = (
        P("fs", "sp", None),
        P(),
        P("fs", "tp"),
        P("fs", "tp"),
        P(),
        P("fs", "tp"),
        P("fs", "tp"),
        P("fs", "tp"),
        P(),
        P(),
        P(),
        P(),
        P("fs", "tp"),
        P("fs", "tp"),
        P(None, "tp"),
        P("tp"),
        P("tp"),
        P("tp", "fs"),
        P("tp", "fs"),
    )
    out_specs = P("fs", "sp", None)
    return jax.shard_map(local, mesh=mesh, in_specs=in_specs, out_specs=out_specs, check_vma=False)
```

```python
import functools

import jax
import jax.numpy as jnp
from jax import lax
from jax.experimental import pallas as pl
from jax.experimental.pallas import tpu as pltpu
from jax.sharding import PartitionSpec as P

MESH_ID = pl.DeviceIdType.MESH

QK_NOPE = 64
QK_ROPE = 32
V_DIM = 64
CONV_W = 1024
SEG = 64
QK_DIM = 96


epsilon = 1e-06
rope_base = 10000.0
masked_score = -1e30


def norm_rows(matrix, scale_vector):
    return (
        matrix
        * lax.rsqrt(jnp.mean(matrix * matrix, axis=-1, keepdims=True) + epsilon)
        * scale_vector
    )


def rope_tables(positions):
    inverse_freq = 1.0 / rope_base ** (jnp.arange(0, QK_ROPE, 2, dtype=jnp.float32) / QK_ROPE)
    angles = positions.astype(jnp.float32)[:, None] * inverse_freq[None, :]
    return (jnp.cos(angles)[:, None, :], jnp.sin(angles)[:, None, :])


def rotate(matrix, cosine_table, sine_table):
    half_width = matrix.shape[-1] // 2
    front_half = matrix[..., :half_width]
    back_half = matrix[..., half_width:]
    return jnp.concatenate(
        [
            front_half * cosine_table - back_half * sine_table,
            front_half * sine_table + back_half * cosine_table,
        ],
        axis=-1,
    )


def heads_query(latent, weight, scale_vector, cosine_table, sine_table):
    row_count = latent.shape[0]
    projected = jnp.dot(latent, weight, preferred_element_type=jnp.float32)
    projected = norm_rows(
        projected.reshape(row_count, weight.shape[1] // QK_DIM, QK_DIM), scale_vector
    )
    turned = rotate(projected[..., QK_NOPE:], cosine_table, sine_table)
    return jnp.concatenate([projected[..., :QK_NOPE], turned], axis=-1).astype(jnp.bfloat16)


def heads_key(latent, rope_rows, weight, scale_vector, cosine_table, sine_table):
    row_count = latent.shape[0]
    head_count = weight.shape[1] // QK_NOPE
    nope_part = jnp.dot(latent, weight, preferred_element_type=jnp.float32).reshape(
        row_count, head_count, QK_NOPE
    )
    shared = jnp.broadcast_to(
        rope_rows.astype(jnp.float32)[:, None, :], (row_count, head_count, QK_ROPE)
    )
    joined = norm_rows(jnp.concatenate([nope_part, shared], axis=-1), scale_vector)
    turned = rotate(joined[..., QK_NOPE:], cosine_table, sine_table)
    return jnp.concatenate([joined[..., :QK_NOPE], turned], axis=-1).astype(jnp.bfloat16)


RIM = 32


def relayed_rows(rows, paired):
    return (rows * 3 // 8) // 16 * 16 if paired else 0


def gather_kernel(
    sizes,
    x_ref, gain_ref, rope_ref, taps_ref, cgain_ref, cshift_ref,
    qd, md, cv, cg, qu, ku, vu, ho, co,
    lq_all, lm_all, rr_all, conv_ref, qu_all, ku_all, vu_all, ho_all, co_all,
    qd_all, md_all, cv_all, cg_all, normed, acc_q, acc_m, acc_v, acc_g, ext, tail, rim,
    sums, stats, stats_all,
    send_d, recv_d, send_r, recv_r, send_z, recv_z, local_sem, rim_sem,
    sp_send, sp_recv, rr_send, rr_recv, tp_send, tp_recv,
):
    n_fs, n_sp, n_tp = sizes
    paired = n_sp % 2 == 0
    f = lax.axis_index("fs")
    s = lax.axis_index("sp")
    t = lax.axis_index("tp")
    parity = lax.rem(s, 2)
    partner = s + 1 - 2 * parity

    barrier = pltpu.get_barrier_semaphore()
    for axis, at, count in (("fs", f, n_fs), ("sp", s, n_sp), ("tp", t, n_tp)):
        for k in range(1, count):
            pl.semaphore_signal(
                barrier, inc=1, device_id={axis: lax.rem(at + k, count)}, device_id_type=MESH_ID
            )
    pl.semaphore_wait(barrier, n_fs + n_sp + n_tp - 3)

    jobs = [
        (qd, qd_all, 0), (md, md_all, 0), (cv, cv_all, 0), (cg, cg_all, 0),
        (qu, qu_all, 0), (ku, ku_all, 0), (vu, vu_all, 0), (ho, ho_all, 1), (co, co_all, 1),
    ]
    last = len(jobs) - 1

    def place(whole, shard, dim, owner, start, count):
        rows, cols = shard.shape
        if dim == 0:
            return whole.at[pl.ds(pl.multiple_of(owner * rows + start, 16), count), :]
        return whole.at[
            pl.ds(pl.multiple_of(start, 16), count),
            pl.ds(pl.multiple_of(owner * cols, 128), cols),
        ]

    square = n_fs == 4
    if square:
        near_x = f + 1 - 2 * lax.rem(f, 2)
        near_y = lax.rem(f + 2, 4)
        far = lax.rem(near_x + 2, 4)
        targets = sources = [near_x, near_y]
    else:
        targets = [lax.rem(f + k, n_fs) for k in range(1, n_fs)]
        sources = [lax.rem(f + n_fs - k, n_fs) for k in range(1, n_fs)]

    direct, far_copies, over_sp, own = [], [], [], []
    for a, (shard, whole, dim) in enumerate(jobs):
        rows = shard.shape[0]
        less = 0 if a == last else relayed_rows(rows, paired)
        start = parity * less
        count = rows - less
        direct.append([
            pltpu.make_async_remote_copy(
                src_ref=shard.at[pl.ds(pl.multiple_of(start, 16), count), :],
                dst_ref=place(whole, shard, dim, f, start, count),
                send_sem=send_d.at[a, k], recv_sem=recv_d.at[a, k],
                device_id={"fs": target}, device_id_type=MESH_ID,
            )
            for k, target in enumerate(targets)
        ])
        halves = []
        if square:
            half = (count // 2 + 15) // 16 * 16
            for k, (owner, target, begin, size) in enumerate((
                (near_y, near_x, start, half), (near_x, near_y, start + half, count - half)
            )):
                piece = place(whole, shard, dim, owner, begin, size)
                halves.append(pltpu.make_async_remote_copy(
                    src_ref=piece, dst_ref=piece,
                    send_sem=send_r.at[a, k], recv_sem=recv_r.at[a, k],
                    device_id={"fs": target}, device_id_type=MESH_ID,
                ))
        far_copies.append(halves)
        across = []
        if less:
            lack = parity * (rows - less)
            for k, owner in enumerate(sources + ([far] if square else [])):
                piece = place(whole, shard, dim, owner, lack, less)
                across.append(pltpu.make_async_remote_copy(
                    src_ref=piece, dst_ref=piece,
                    send_sem=send_z.at[a, k], recv_sem=recv_z.at[a, k],
                    device_id={"sp": partner}, device_id_type=MESH_ID,
                ))
        over_sp.append(across)
        own.append(pltpu.make_async_copy(
            shard, place(whole, shard, dim, f, 0, rows), local_sem.at[a]
        ))

    def begin_array(a):
        if a <= last:
            for copy in direct[a]:
                copy.start()

    def finish_far(a):
        for copy in far_copies[a]:
            copy.wait_recv()
        for copy in over_sp[a][len(sources):]:
            copy.start()

    def tick(a):
        for copy in direct[a]:
            copy.wait_recv()
        for copy in far_copies[a]:
            copy.start()
        begin_array(a + 3)
        for copy in over_sp[a][: len(sources)]:
            copy.start()
        if a >= 1:
            finish_far(a - 1)

    def complete(a):
        own[a].wait()
        for copy in over_sp[a]:
            copy.wait_recv()

    for a in range(3):
        begin_array(a)
    for copy in own:
        copy.start()

    rows = x_ref.shape[0]
    part = 32

    @pl.loop(0, rows // part)
    def _(i):
        at = pl.ds(pl.multiple_of(i * part, part), part)
        x = x_ref[at, :].astype(jnp.float32)
        scale = lax.rsqrt(jnp.mean(x * x, axis=-1, keepdims=True) + epsilon)
        normed[at, :] = (x * scale * gain_ref[...]).astype(jnp.bfloat16)

    depth = qd.shape[0]

    def project(weight, acc):
        acc[...] = jnp.zeros_like(acc)

        @pl.loop(0, n_fs)
        def _(i):
            at = pl.ds(pl.multiple_of(i * depth, depth), depth)
            acc[...] += jnp.dot(
                normed[:, at], weight[at, :], preferred_element_type=jnp.float32
            )

    mine = pl.ds(pl.multiple_of(s * rows, 16), rows)
    rr_all[mine, :] = jnp.dot(
        normed[...], rope_ref[...], preferred_element_type=jnp.float32
    ).astype(jnp.bfloat16)
    tick(0)
    tick(1)
    tick(2)
    complete(0)
    project(qd_all, acc_q)
    lq_all[t, :, :] = acc_q[...].astype(jnp.bfloat16)
    tick(3)
    complete(1)
    project(md_all, acc_m)
    lm_all[t, mine, :] = acc_m[...].astype(jnp.bfloat16)
    tick(4)
    complete(2)
    project(cv_all, acc_v)

    exchanges, passes = [], []
    for k in range(1, n_sp):
        peer = {"sp": lax.rem(s + k, n_sp)}
        exchanges.append(pltpu.make_async_remote_copy(
            src_ref=lm_all.at[t, mine, :], dst_ref=lm_all.at[t, mine, :],
            send_sem=sp_send.at[k - 1], recv_sem=sp_recv.at[k - 1],
            device_id=peer, device_id_type=MESH_ID,
        ))
        exchanges.append(pltpu.make_async_remote_copy(
            src_ref=rr_all.at[mine, :], dst_ref=rr_all.at[mine, :],
            send_sem=rr_send.at[k - 1], recv_sem=rr_recv.at[k - 1],
            device_id=peer, device_id_type=MESH_ID,
        ))
    tp_peers = [{"tp": lax.rem(t + k, n_tp)} for k in range(1, n_tp)]

    def to_tp(kind, source, landing):
        return [
            pltpu.make_async_remote_copy(
                src_ref=source, dst_ref=landing(k),
                send_sem=tp_send.at[kind, k], recv_sem=tp_recv.at[kind, k],
                device_id=peer, device_id_type=MESH_ID,
            )
            for k, peer in enumerate(tp_peers)
        ]

    query_copies = to_tp(0, lq_all.at[t], lambda k: lq_all.at[t])
    memory_copies = to_tp(1, lm_all.at[t], lambda k: lm_all.at[t])
    stat_copies = to_tp(2, stats, lambda k: stats_all.at[k])
    for copy in exchanges + query_copies:
        copy.start()
    tick(5)
    complete(3)
    project(cg_all, acc_g)

    @pl.loop(0, rows // part)
    def _(i):
        at = pl.ds(pl.multiple_of(i * part, part), part)
        gated = (acc_v[at, :] * jax.nn.sigmoid(acc_g[at, :])).astype(jnp.bfloat16)
        ext[pl.ds(pl.multiple_of(RIM + i * part, part), part), :] = gated.astype(jnp.float32)

    tail[...] = ext[pl.ds(rows, RIM), :].astype(jnp.bfloat16)
    rim_copy = pltpu.make_async_remote_copy(
        src_ref=tail, dst_ref=rim, send_sem=rim_sem.at[0], recv_sem=rim_sem.at[1],
        device_id={"sp": lax.rem(s + 1, n_sp)}, device_id_type=MESH_ID,
    )
    tick(6)

    @pl.when(s < n_sp - 1)
    def _():
        rim_copy.start()

    for copy in exchanges:
        copy.wait_recv()
    for copy in memory_copies:
        copy.start()

    @pl.when(s > 0)
    def _():
        rim_copy.wait_recv()
        ext[pl.ds(0, RIM), :] = rim[...].astype(jnp.float32)

    @pl.when(s == 0)
    def _():
        ext[pl.ds(0, RIM), :] = jnp.zeros((RIM, ext.shape[1]), jnp.float32)

    tap_count = taps_ref.shape[0]
    block = 64

    @pl.loop(0, ext.shape[1] // 128)
    def _(c):
        cols = pl.ds(pl.multiple_of(c * 128, 128), 128)
        taps = taps_ref[:, cols].astype(jnp.float32)
        for r in range(0, rows, block):
            total = jnp.zeros((block, 128), jnp.float32)
            for j in range(tap_count):
                total = total + ext[
                    pl.ds(r + RIM - (tap_count - 1) + j, block), cols
                ] * taps[j : j + 1, :]
            sums[pl.ds(r, block), cols] = total

    @pl.loop(0, rows // part)
    def _(i):
        begin = pl.multiple_of(i * part, part)
        values = sums[pl.ds(begin, part), :]
        stats[pl.ds(begin, part), :] = jnp.broadcast_to(
            jnp.sum(values, axis=1, keepdims=True), (part, 128)
        )
        stats[pl.ds(pl.multiple_of(rows + begin, part), part), :] = jnp.broadcast_to(
            jnp.sum(values * values, axis=1, keepdims=True), (part, 128)
        )

    tick(7)
    for copy in stat_copies:
        copy.start()
    tick(8)
    for copy in stat_copies:
        copy.wait_recv()

    channels = ext.shape[1] * n_tp

    @pl.loop(0, rows // part)
    def _(i):
        begin = pl.multiple_of(i * part, part)
        upper = pl.ds(begin, part)
        lower = pl.ds(pl.multiple_of(rows + begin, part), part)
        total, squares = stats[upper, :], stats[lower, :]
        for k in range(n_tp - 1):
            total = total + stats_all[k, upper, :]
            squares = squares + stats_all[k, lower, :]
        mean = total[:, :1] / channels
        spread = squares[:, :1] / channels - mean * mean
        shaped = (sums[upper, :] - mean) * lax.rsqrt(spread + epsilon)
        conv_ref[upper, :] = jax.nn.silu(
            shaped * cgain_ref[...] + cshift_ref[...]
        ).astype(jnp.bfloat16)

    finish_far(last)
    for a in range(4, last + 1):
        complete(a)
    for copy in query_copies + memory_copies:
        copy.wait_recv()
    for group in direct + far_copies + over_sp:
        for copy in group:
            copy.wait_send()
    for copy in exchanges + query_copies + memory_copies + stat_copies:
        copy.wait_send()

    @pl.when(s < n_sp - 1)
    def _():
        rim_copy.wait_send()


def gather_and_project(
    sizes, x, mix_gain, rope_weight, taps, channel_gain, channel_shift,
    qd, md, cv, cg, qu, ku, vu, ho, co,
):
    n_fs, n_sp, n_tp = sizes
    rows = x.shape[0]
    bf16, f32 = jnp.bfloat16, jnp.float32
    vmem = pl.BlockSpec(memory_space=pltpu.VMEM)
    hbm = pl.BlockSpec(memory_space=pl.ANY)

    def whole(w, dim=0):
        return (w.shape[0] * n_fs, w.shape[1]) if dim == 0 else (w.shape[0], w.shape[1] * n_fs)

    out_shapes = [
        ((n_tp, rows, qd.shape[1]), bf16), ((n_tp, n_sp * rows, md.shape[1]), bf16),
        ((n_sp * rows, rope_weight.shape[1]), bf16), ((rows, cv.shape[1]), bf16),
        (whole(qu), bf16), (whole(ku), bf16), (whole(vu), bf16),
        (whole(ho, 1), bf16), (whole(co, 1), bf16),
    ]
    dma = pltpu.SemaphoreType.DMA
    tp_others = max(n_tp - 1, 1)
    sp_others = max(n_sp - 1, 1)
    return pl.pallas_call(
        functools.partial(gather_kernel, sizes),
        out_shape=[jax.ShapeDtypeStruct(*o) for o in out_shapes],
        in_specs=[vmem] * 6 + [hbm] * 9,
        out_specs=[vmem] * 9,
        scratch_shapes=[
            pltpu.VMEM(whole(qd), bf16), pltpu.VMEM(whole(md), bf16),
            pltpu.VMEM(whole(cv), bf16), pltpu.VMEM(whole(cg), bf16),
            pltpu.VMEM(x.shape, bf16), pltpu.VMEM((rows, qd.shape[1]), f32),
            pltpu.VMEM((rows, md.shape[1]), f32),
            pltpu.VMEM((rows, cv.shape[1]), f32), pltpu.VMEM((rows, cv.shape[1]), f32),
            pltpu.VMEM((rows + RIM, cv.shape[1]), f32),
            pltpu.VMEM((RIM, cv.shape[1]), bf16), pltpu.VMEM((RIM, cv.shape[1]), bf16),
            pltpu.VMEM((rows, cv.shape[1]), f32), pltpu.VMEM((2 * rows, 128), f32),
            pltpu.VMEM((tp_others, 2 * rows, 128), f32),
            dma((9, n_fs - 1)), dma((9, n_fs - 1)), dma((9, 2)), dma((9, 2)),
            dma((9, n_fs - 1)), dma((9, n_fs - 1)), dma((9,)), dma((2,)),
            dma((sp_others,)), dma((sp_others,)), dma((sp_others,)), dma((sp_others,)),
            dma((3, tp_others)), dma((3, tp_others)),
        ],
        compiler_params=pltpu.CompilerParams(
            collective_id=0, has_side_effects=True, vmem_limit_bytes=56 * 1024 * 1024
        ),
    )(
        x, mix_gain[None, :], rope_weight, taps, channel_gain[None, :], channel_shift[None, :],
        qd, md, cv, cg, qu, ku, vu, ho, co,
    )


def key_block(key_count):
    block_size = key_count
    while block_size > 2048 and block_size % 2 == 0:
        block_size = block_size // 2
    return block_size


def sum_groups(partial):
    count = lax.axis_size("tp")
    if count != 2:
        return lax.psum(partial, "tp")
    other = lax.ppermute(partial, "tp", [(0, 1), (1, 0)])
    return (partial.astype(jnp.float32) + other.astype(jnp.float32)).astype(jnp.bfloat16)


def local(
    tokens,
    mix_gain,
    query_down,
    memory_down,
    rope_weight,
    query_up,
    key_up,
    value_up,
    latent_gain,
    memory_gain,
    query_gain,
    key_gain,
    conv_value,
    conv_gate,
    conv_kernel,
    channel_gain,
    channel_shift,
    heads_out,
    conv_out,
):
    own_rows = tokens[0]
    (
        query_parts, memory_parts, rope_piece, conv_result,
        up_query, up_keys, up_values, out_heads, out_conv,
    ) = gather_and_project(
        (lax.axis_size("fs"), lax.axis_size("sp"), lax.axis_size("tp")),
        own_rows, mix_gain, rope_weight, conv_kernel, channel_gain, channel_shift,
        query_down, memory_down, conv_value, conv_gate,
        query_up, key_up, value_up, heads_out, conv_out,
    )
    row_count = own_rows.shape[0]
    whole_query = jnp.concatenate(list(query_parts), axis=1)
    whole_memory = jnp.concatenate(list(memory_parts), axis=1)
    query_normed = norm_rows(whole_query.astype(jnp.float32), latent_gain).astype(jnp.bfloat16)
    memory_piece = norm_rows(whole_memory.astype(jnp.float32), memory_gain).astype(jnp.bfloat16)
    positions = lax.axis_index("sp") * row_count + jnp.arange(row_count, dtype=jnp.int32)
    cosine_table, sine_table = rope_tables(positions)
    queries = heads_query(query_normed, up_query, query_gain, cosine_table, sine_table)
    head_count = queries.shape[1]
    query_segment = positions // SEG
    score_scale = QK_DIM ** (-0.5)
    def attend(state_carry, key_rows, value_rows, key_pos):
        running_max, row_total, weighted = state_carry
        scores = (
            jnp.einsum("qhd,khd->qhk", queries, key_rows, preferred_element_type=jnp.float32)
            * score_scale
        )
        allowed = ((key_pos // SEG)[None, :] <= query_segment[:, None])[:, None, :]
        scores = jnp.where(allowed, scores, masked_score)
        new_max = jnp.maximum(running_max, jnp.max(scores, axis=2))
        weights = jnp.where(allowed, jnp.exp(scores - new_max[:, :, None]), 0.0)
        factor = jnp.exp(running_max - new_max)
        row_total = row_total * factor + jnp.sum(weights, axis=2)
        weighted = weighted * factor[:, :, None] + jnp.einsum(
            "qhk,khd->qhd",
            weights.astype(jnp.bfloat16),
            value_rows,
            preferred_element_type=jnp.float32,
        )
        return (new_max, row_total, weighted)

    initial = (
        jnp.full((row_count, head_count), masked_score, jnp.float32),
        jnp.zeros((row_count, head_count), jnp.float32),
        jnp.zeros((row_count, head_count, V_DIM), jnp.float32),
    )
    def block_keys(block_start, block_size):
        memory_block = lax.dynamic_slice_in_dim(memory_piece, block_start, block_size, 0)
        rope_block = lax.dynamic_slice_in_dim(rope_piece, block_start, block_size, 0)
        key_pos = block_start + jnp.arange(block_size, dtype=jnp.int32)
        cosine_keys, sine_keys = rope_tables(key_pos)
        key_rows = heads_key(memory_block, rope_block, up_keys, key_gain, cosine_keys, sine_keys)
        value_rows = (
            jnp.dot(memory_block, up_values, preferred_element_type=jnp.float32)
            .astype(jnp.bfloat16)
            .reshape(block_size, head_count, V_DIM)
        )
        return (key_rows, value_rows, key_pos)

    key_count = memory_piece.shape[0]
    block_size = key_block(key_count)

    def step(block_index, running):
        key_rows, value_rows, key_pos = block_keys(block_index * block_size, block_size)
        return attend(running, key_rows, value_rows, key_pos)

    final_state = lax.fori_loop(0, key_count // block_size, step, initial)
    running_max, row_total, weighted = final_state
    attention = (
        (weighted / row_total[:, :, None])
        .astype(jnp.bfloat16)
        .reshape(row_count, head_count * V_DIM)
    )
    mixer_rows = jnp.concatenate([attention, conv_result], axis=1)
    out_weight = jnp.concatenate([out_heads, out_conv], axis=0)
    partial_sum = jnp.dot(mixer_rows, out_weight, preferred_element_type=jnp.float32)
    mixed = sum_groups(partial_sum.astype(jnp.bfloat16))
    return mixed[None]


def solution(mesh):
    in_specs = (
        P("fs", "sp", None),
        P(),
        P("fs", "tp"),
        P("fs", "tp"),
        P(),
        P("fs", "tp"),
        P("fs", "tp"),
        P("fs", "tp"),
        P(),
        P(),
        P(),
        P(),
        P("fs", "tp"),
        P("fs", "tp"),
        P(None, "tp"),
        P("tp"),
        P("tp"),
        P("tp", "fs"),
        P("tp", "fs"),
    )
    out_specs = P("fs", "sp", None)
    return jax.shard_map(local, mesh=mesh, in_specs=in_specs, out_specs=out_specs, check_vma=False)
```

```python
import functools

import jax
import jax.numpy as jnp
from jax import lax
from jax.experimental import pallas as pl
from jax.experimental.pallas import tpu as pltpu
from jax.sharding import PartitionSpec as P

MESH_ID = pl.DeviceIdType.MESH

QK_NOPE = 64
QK_ROPE = 32
V_DIM = 64
CONV_W = 1024
SEG = 64
QK_DIM = 96


epsilon = 1e-06
rope_base = 10000.0
masked_score = -1e30


def norm_rows(matrix, scale_vector):
    return (
        matrix
        * lax.rsqrt(jnp.mean(matrix * matrix, axis=-1, keepdims=True) + epsilon)
        * scale_vector
    )


def rope_tables(positions):
    inverse_freq = 1.0 / rope_base ** (jnp.arange(0, QK_ROPE, 2, dtype=jnp.float32) / QK_ROPE)
    angles = positions.astype(jnp.float32)[:, None] * inverse_freq[None, :]
    return (jnp.cos(angles)[:, None, :], jnp.sin(angles)[:, None, :])


def rotate(matrix, cosine_table, sine_table):
    half_width = matrix.shape[-1] // 2
    front_half = matrix[..., :half_width]
    back_half = matrix[..., half_width:]
    return jnp.concatenate(
        [
            front_half * cosine_table - back_half * sine_table,
            front_half * sine_table + back_half * cosine_table,
        ],
        axis=-1,
    )


def heads_query(latent, weight, scale_vector, cosine_table, sine_table):
    row_count = latent.shape[0]
    projected = jnp.dot(latent, weight, preferred_element_type=jnp.float32)
    projected = norm_rows(
        projected.reshape(row_count, weight.shape[1] // QK_DIM, QK_DIM), scale_vector
    )
    turned = rotate(projected[..., QK_NOPE:], cosine_table, sine_table)
    return jnp.concatenate([projected[..., :QK_NOPE], turned], axis=-1).astype(jnp.bfloat16)


def heads_key(latent, rope_rows, weight, scale_vector, cosine_table, sine_table):
    row_count = latent.shape[0]
    head_count = weight.shape[1] // QK_NOPE
    nope_part = jnp.dot(latent, weight, preferred_element_type=jnp.float32).reshape(
        row_count, head_count, QK_NOPE
    )
    shared = jnp.broadcast_to(
        rope_rows.astype(jnp.float32)[:, None, :], (row_count, head_count, QK_ROPE)
    )
    joined = norm_rows(jnp.concatenate([nope_part, shared], axis=-1), scale_vector)
    turned = rotate(joined[..., QK_NOPE:], cosine_table, sine_table)
    return jnp.concatenate([joined[..., :QK_NOPE], turned], axis=-1).astype(jnp.bfloat16)


RIM = 32


def relayed_rows(rows, paired):
    return (rows * 5 // 16) // 16 * 16 if paired else 0


def gather_kernel(
    sizes,
    x_ref, gain_ref, rope_ref, taps_ref, cgain_ref, cshift_ref,
    qd, md, cv, cg, qu, ku, vu, ho, co,
    lq_all, lm_all, rr_all, conv_ref, qu_all, ku_all, vu_all, ho_all, co_all,
    qd_all, md_all, cv_all, cg_all, normed, acc_q, acc_m, acc_v, acc_g, ext, tail, rim,
    sums, stats, stats_all,
    send_d, recv_d, send_r, recv_r, send_z, recv_z, local_sem, rim_sem,
    sp_send, sp_recv, rr_send, rr_recv, tp_send, tp_recv,
):
    n_fs, n_sp, n_tp = sizes
    paired = n_sp % 2 == 0
    f = lax.axis_index("fs")
    s = lax.axis_index("sp")
    t = lax.axis_index("tp")
    parity = lax.rem(s, 2)
    partner = s + 1 - 2 * parity

    barrier = pltpu.get_barrier_semaphore()
    for axis, at, count in (("fs", f, n_fs), ("sp", s, n_sp), ("tp", t, n_tp)):
        for k in range(1, count):
            pl.semaphore_signal(
                barrier, inc=1, device_id={axis: lax.rem(at + k, count)}, device_id_type=MESH_ID
            )
    pl.semaphore_wait(barrier, n_fs + n_sp + n_tp - 3)

    jobs = [
        (qd, qd_all, 0), (md, md_all, 0), (cv, cv_all, 0), (cg, cg_all, 0),
        (qu, qu_all, 0), (ku, ku_all, 0), (vu, vu_all, 0), (ho, ho_all, 1), (co, co_all, 1),
    ]
    last = len(jobs) - 1
    ahead = 4

    def place(whole, shard, dim, owner, start, count):
        rows, cols = shard.shape
        if dim == 0:
            return whole.at[pl.ds(pl.multiple_of(owner * rows + start, 16), count), :]
        return whole.at[
            pl.ds(pl.multiple_of(start, 16), count),
            pl.ds(pl.multiple_of(owner * cols, 128), cols),
        ]

    square = n_fs == 4
    if square:
        near_x = f + 1 - 2 * lax.rem(f, 2)
        near_y = lax.rem(f + 2, 4)
        far = lax.rem(near_x + 2, 4)
        targets = sources = [near_x, near_y]
    else:
        targets = [lax.rem(f + k, n_fs) for k in range(1, n_fs)]
        sources = [lax.rem(f + n_fs - k, n_fs) for k in range(1, n_fs)]

    direct, far_copies, over_sp, own = [], [], [], []
    for a, (shard, whole, dim) in enumerate(jobs):
        rows = shard.shape[0]
        less = 0 if a == last else relayed_rows(rows, paired)
        start = parity * less
        count = rows - less
        direct.append([
            pltpu.make_async_remote_copy(
                src_ref=shard.at[pl.ds(pl.multiple_of(start, 16), count), :],
                dst_ref=place(whole, shard, dim, f, start, count),
                send_sem=send_d.at[a, k], recv_sem=recv_d.at[a, k],
                device_id={"fs": target}, device_id_type=MESH_ID,
            )
            for k, target in enumerate(targets)
        ])
        halves = []
        if square:
            half = (count // 2 + 15) // 16 * 16
            for k, (owner, target, begin, size) in enumerate((
                (near_y, near_x, start, half), (near_x, near_y, start + half, count - half)
            )):
                piece = place(whole, shard, dim, owner, begin, size)
                halves.append(pltpu.make_async_remote_copy(
                    src_ref=piece, dst_ref=piece,
                    send_sem=send_r.at[a, k], recv_sem=recv_r.at[a, k],
                    device_id={"fs": target}, device_id_type=MESH_ID,
                ))
        far_copies.append(halves)
        across = []
        if less:
            lack = parity * (rows - less)
            for k, owner in enumerate(sources + ([far] if square else [])):
                piece = place(whole, shard, dim, owner, lack, less)
                across.append(pltpu.make_async_remote_copy(
                    src_ref=piece, dst_ref=piece,
                    send_sem=send_z.at[a, k], recv_sem=recv_z.at[a, k],
                    device_id={"sp": partner}, device_id_type=MESH_ID,
                ))
        over_sp.append(across)
        own.append(pltpu.make_async_copy(
            shard, place(whole, shard, dim, f, 0, rows), local_sem.at[a]
        ))

    def begin_array(a):
        if a <= last:
            for copy in direct[a]:
                copy.start()

    def finish_far(a):
        for copy in far_copies[a]:
            copy.wait_recv()
        for copy in over_sp[a][len(sources):]:
            copy.start()

    def tick(a):
        for copy in direct[a]:
            copy.wait_recv()
        for copy in far_copies[a]:
            copy.start()
        begin_array(a + ahead)
        for copy in over_sp[a][: len(sources)]:
            copy.start()
        if a >= 1:
            finish_far(a - 1)

    def complete(a):
        own[a].wait()
        for copy in over_sp[a]:
            copy.wait_recv()

    for a in range(ahead):
        begin_array(a)
    for copy in own:
        copy.start()

    rows = x_ref.shape[0]
    part = 32

    @pl.loop(0, rows // part)
    def _(i):
        at = pl.ds(pl.multiple_of(i * part, part), part)
        x = x_ref[at, :].astype(jnp.float32)
        scale = lax.rsqrt(jnp.mean(x * x, axis=-1, keepdims=True) + epsilon)
        normed[at, :] = (x * scale * gain_ref[...]).astype(jnp.bfloat16)

    depth = qd.shape[0]

    def project(weight, acc):
        acc[...] = jnp.zeros_like(acc)

        @pl.loop(0, n_fs)
        def _(i):
            at = pl.ds(pl.multiple_of(i * depth, depth), depth)
            acc[...] += jnp.dot(
                normed[:, at], weight[at, :], preferred_element_type=jnp.float32
            )

    mine = pl.ds(pl.multiple_of(s * rows, 16), rows)
    rr_all[mine, :] = jnp.dot(
        normed[...], rope_ref[...], preferred_element_type=jnp.float32
    ).astype(jnp.bfloat16)
    tick(0)
    tick(1)
    tick(2)
    complete(0)
    project(qd_all, acc_q)
    lq_all[t, :, :] = acc_q[...].astype(jnp.bfloat16)
    tick(3)
    complete(1)
    project(md_all, acc_m)
    lm_all[t, mine, :] = acc_m[...].astype(jnp.bfloat16)
    tick(4)
    complete(2)
    project(cv_all, acc_v)

    exchanges, passes = [], []
    for k in range(1, n_sp):
        peer = {"sp": lax.rem(s + k, n_sp)}
        exchanges.append(pltpu.make_async_remote_copy(
            src_ref=lm_all.at[t, mine, :], dst_ref=lm_all.at[t, mine, :],
            send_sem=sp_send.at[k - 1], recv_sem=sp_recv.at[k - 1],
            device_id=peer, device_id_type=MESH_ID,
        ))
        exchanges.append(pltpu.make_async_remote_copy(
            src_ref=rr_all.at[mine, :], dst_ref=rr_all.at[mine, :],
            send_sem=rr_send.at[k - 1], recv_sem=rr_recv.at[k - 1],
            device_id=peer, device_id_type=MESH_ID,
        ))
    tp_peers = [{"tp": lax.rem(t + k, n_tp)} for k in range(1, n_tp)]

    def to_tp(kind, source, landing):
        return [
            pltpu.make_async_remote_copy(
                src_ref=source, dst_ref=landing(k),
                send_sem=tp_send.at[kind, k], recv_sem=tp_recv.at[kind, k],
                device_id=peer, device_id_type=MESH_ID,
            )
            for k, peer in enumerate(tp_peers)
        ]

    query_copies = to_tp(0, lq_all.at[t], lambda k: lq_all.at[t])
    memory_copies = to_tp(1, lm_all.at[t], lambda k: lm_all.at[t])
    stat_copies = to_tp(2, stats, lambda k: stats_all.at[k])
    for copy in exchanges + query_copies:
        copy.start()
    tick(5)
    complete(3)
    project(cg_all, acc_g)

    @pl.loop(0, rows // part)
    def _(i):
        at = pl.ds(pl.multiple_of(i * part, part), part)
        gated = (acc_v[at, :] * jax.nn.sigmoid(acc_g[at, :])).astype(jnp.bfloat16)
        ext[pl.ds(pl.multiple_of(RIM + i * part, part), part), :] = gated.astype(jnp.float32)

    tail[...] = ext[pl.ds(rows, RIM), :].astype(jnp.bfloat16)
    rim_copy = pltpu.make_async_remote_copy(
        src_ref=tail, dst_ref=rim, send_sem=rim_sem.at[0], recv_sem=rim_sem.at[1],
        device_id={"sp": lax.rem(s + 1, n_sp)}, device_id_type=MESH_ID,
    )
    tick(6)

    @pl.when(s < n_sp - 1)
    def _():
        rim_copy.start()

    for copy in exchanges:
        copy.wait_recv()
    for copy in memory_copies:
        copy.start()

    @pl.when(s > 0)
    def _():
        rim_copy.wait_recv()
        ext[pl.ds(0, RIM), :] = rim[...].astype(jnp.float32)

    @pl.when(s == 0)
    def _():
        ext[pl.ds(0, RIM), :] = jnp.zeros((RIM, ext.shape[1]), jnp.float32)

    tap_count = taps_ref.shape[0]
    block = 64

    def convolve(c):
        cols = pl.ds(pl.multiple_of(c * 128, 128), 128)
        taps = taps_ref[:, cols].astype(jnp.float32)
        for r in range(0, rows, block):
            total = jnp.zeros((block, 128), jnp.float32)
            for j in range(tap_count):
                total = total + ext[
                    pl.ds(r + RIM - (tap_count - 1) + j, block), cols
                ] * taps[j : j + 1, :]
            sums[pl.ds(r, block), cols] = total

    tiles = ext.shape[1] // 128
    pl.loop(0, tiles // 2)(convolve)
    tick(7)
    pl.loop(tiles // 2, tiles)(convolve)

    @pl.loop(0, rows // part)
    def _(i):
        begin = pl.multiple_of(i * part, part)
        values = sums[pl.ds(begin, part), :]
        stats[pl.ds(begin, part), :] = jnp.broadcast_to(
            jnp.sum(values, axis=1, keepdims=True), (part, 128)
        )
        stats[pl.ds(pl.multiple_of(rows + begin, part), part), :] = jnp.broadcast_to(
            jnp.sum(values * values, axis=1, keepdims=True), (part, 128)
        )

    tick(8)
    for copy in stat_copies:
        copy.start()
    for copy in stat_copies:
        copy.wait_recv()

    channels = ext.shape[1] * n_tp

    @pl.loop(0, rows // part)
    def _(i):
        begin = pl.multiple_of(i * part, part)
        upper = pl.ds(begin, part)
        lower = pl.ds(pl.multiple_of(rows + begin, part), part)
        total, squares = stats[upper, :], stats[lower, :]
        for k in range(n_tp - 1):
            total = total + stats_all[k, upper, :]
            squares = squares + stats_all[k, lower, :]
        mean = total[:, :1] / channels
        spread = squares[:, :1] / channels - mean * mean
        shaped = (sums[upper, :] - mean) * lax.rsqrt(spread + epsilon)
        conv_ref[upper, :] = jax.nn.silu(
            shaped * cgain_ref[...] + cshift_ref[...]
        ).astype(jnp.bfloat16)

    finish_far(last)
    for a in range(4, last + 1):
        complete(a)
    for copy in query_copies + memory_copies:
        copy.wait_recv()
    for group in direct + far_copies + over_sp:
        for copy in group:
            copy.wait_send()
    for copy in exchanges + query_copies + memory_copies + stat_copies:
        copy.wait_send()

    @pl.when(s < n_sp - 1)
    def _():
        rim_copy.wait_send()


def gather_and_project(
    sizes, x, mix_gain, rope_weight, taps, channel_gain, channel_shift,
    qd, md, cv, cg, qu, ku, vu, ho, co,
):
    n_fs, n_sp, n_tp = sizes
    rows = x.shape[0]
    bf16, f32 = jnp.bfloat16, jnp.float32
    vmem = pl.BlockSpec(memory_space=pltpu.VMEM)
    hbm = pl.BlockSpec(memory_space=pl.ANY)

    def whole(w, dim=0):
        return (w.shape[0] * n_fs, w.shape[1]) if dim == 0 else (w.shape[0], w.shape[1] * n_fs)

    out_shapes = [
        ((n_tp, rows, qd.shape[1]), bf16), ((n_tp, n_sp * rows, md.shape[1]), bf16),
        ((n_sp * rows, rope_weight.shape[1]), bf16), ((rows, cv.shape[1]), bf16),
        (whole(qu), bf16), (whole(ku), bf16), (whole(vu), bf16),
        (whole(ho, 1), bf16), (whole(co, 1), bf16),
    ]
    dma = pltpu.SemaphoreType.DMA
    tp_others = max(n_tp - 1, 1)
    sp_others = max(n_sp - 1, 1)
    return pl.pallas_call(
        functools.partial(gather_kernel, sizes),
        out_shape=[jax.ShapeDtypeStruct(*o) for o in out_shapes],
        in_specs=[vmem] * 6 + [hbm] * 9,
        out_specs=[vmem] * 9,
        scratch_shapes=[
            pltpu.VMEM(whole(qd), bf16), pltpu.VMEM(whole(md), bf16),
            pltpu.VMEM(whole(cv), bf16), pltpu.VMEM(whole(cg), bf16),
            pltpu.VMEM(x.shape, bf16), pltpu.VMEM((rows, qd.shape[1]), f32),
            pltpu.VMEM((rows, md.shape[1]), f32),
            pltpu.VMEM((rows, cv.shape[1]), f32), pltpu.VMEM((rows, cv.shape[1]), f32),
            pltpu.VMEM((rows + RIM, cv.shape[1]), f32),
            pltpu.VMEM((RIM, cv.shape[1]), bf16), pltpu.VMEM((RIM, cv.shape[1]), bf16),
            pltpu.VMEM((rows, cv.shape[1]), f32), pltpu.VMEM((2 * rows, 128), f32),
            pltpu.VMEM((tp_others, 2 * rows, 128), f32),
            dma((9, n_fs - 1)), dma((9, n_fs - 1)), dma((9, 2)), dma((9, 2)),
            dma((9, n_fs - 1)), dma((9, n_fs - 1)), dma((9,)), dma((2,)),
            dma((sp_others,)), dma((sp_others,)), dma((sp_others,)), dma((sp_others,)),
            dma((3, tp_others)), dma((3, tp_others)),
        ],
        compiler_params=pltpu.CompilerParams(
            collective_id=0, has_side_effects=True, vmem_limit_bytes=56 * 1024 * 1024
        ),
    )(
        x, mix_gain[None, :], rope_weight, taps, channel_gain[None, :], channel_shift[None, :],
        qd, md, cv, cg, qu, ku, vu, ho, co,
    )


def key_block(key_count):
    block_size = key_count
    while block_size > 2048 and block_size % 2 == 0:
        block_size = block_size // 2
    return block_size


def sum_groups(partial):
    count = lax.axis_size("tp")
    if count != 2:
        return lax.psum(partial, "tp")
    other = lax.ppermute(partial, "tp", [(0, 1), (1, 0)])
    return (partial.astype(jnp.float32) + other.astype(jnp.float32)).astype(jnp.bfloat16)


def local(
    tokens,
    mix_gain,
    query_down,
    memory_down,
    rope_weight,
    query_up,
    key_up,
    value_up,
    latent_gain,
    memory_gain,
    query_gain,
    key_gain,
    conv_value,
    conv_gate,
    conv_kernel,
    channel_gain,
    channel_shift,
    heads_out,
    conv_out,
):
    own_rows = tokens[0]
    (
        query_parts, memory_parts, rope_piece, conv_result,
        up_query, up_keys, up_values, out_heads, out_conv,
    ) = gather_and_project(
        (lax.axis_size("fs"), lax.axis_size("sp"), lax.axis_size("tp")),
        own_rows, mix_gain, rope_weight, conv_kernel, channel_gain, channel_shift,
        query_down, memory_down, conv_value, conv_gate,
        query_up, key_up, value_up, heads_out, conv_out,
    )
    row_count = own_rows.shape[0]
    whole_query = jnp.concatenate(list(query_parts), axis=1)
    whole_memory = jnp.concatenate(list(memory_parts), axis=1)
    query_normed = norm_rows(whole_query.astype(jnp.float32), latent_gain).astype(jnp.bfloat16)
    memory_piece = norm_rows(whole_memory.astype(jnp.float32), memory_gain).astype(jnp.bfloat16)
    positions = lax.axis_index("sp") * row_count + jnp.arange(row_count, dtype=jnp.int32)
    cosine_table, sine_table = rope_tables(positions)
    queries = heads_query(query_normed, up_query, query_gain, cosine_table, sine_table)
    head_count = queries.shape[1]
    query_segment = positions // SEG
    score_scale = QK_DIM ** (-0.5)
    def attend(state_carry, key_rows, value_rows, key_pos):
        running_max, row_total, weighted = state_carry
        scores = (
            jnp.einsum("qhd,khd->qhk", queries, key_rows, preferred_element_type=jnp.float32)
            * score_scale
        )
        allowed = ((key_pos // SEG)[None, :] <= query_segment[:, None])[:, None, :]
        scores = jnp.where(allowed, scores, masked_score)
        new_max = jnp.maximum(running_max, jnp.max(scores, axis=2))
        weights = jnp.where(allowed, jnp.exp(scores - new_max[:, :, None]), 0.0)
        factor = jnp.exp(running_max - new_max)
        row_total = row_total * factor + jnp.sum(weights, axis=2)
        weighted = weighted * factor[:, :, None] + jnp.einsum(
            "qhk,khd->qhd",
            weights.astype(jnp.bfloat16),
            value_rows,
            preferred_element_type=jnp.float32,
        )
        return (new_max, row_total, weighted)

    initial = (
        jnp.full((row_count, head_count), masked_score, jnp.float32),
        jnp.zeros((row_count, head_count), jnp.float32),
        jnp.zeros((row_count, head_count, V_DIM), jnp.float32),
    )
    def block_keys(block_start, block_size):
        memory_block = lax.dynamic_slice_in_dim(memory_piece, block_start, block_size, 0)
        rope_block = lax.dynamic_slice_in_dim(rope_piece, block_start, block_size, 0)
        key_pos = block_start + jnp.arange(block_size, dtype=jnp.int32)
        cosine_keys, sine_keys = rope_tables(key_pos)
        key_rows = heads_key(memory_block, rope_block, up_keys, key_gain, cosine_keys, sine_keys)
        value_rows = (
            jnp.dot(memory_block, up_values, preferred_element_type=jnp.float32)
            .astype(jnp.bfloat16)
            .reshape(block_size, head_count, V_DIM)
        )
        return (key_rows, value_rows, key_pos)

    key_count = memory_piece.shape[0]
    block_size = key_block(key_count)

    def step(block_index, running):
        key_rows, value_rows, key_pos = block_keys(block_index * block_size, block_size)
        return attend(running, key_rows, value_rows, key_pos)

    final_state = lax.fori_loop(0, key_count // block_size, step, initial)
    running_max, row_total, weighted = final_state
    attention = (
        (weighted / row_total[:, :, None])
        .astype(jnp.bfloat16)
        .reshape(row_count, head_count * V_DIM)
    )
    mixer_rows = jnp.concatenate([attention, conv_result], axis=1)
    out_weight = jnp.concatenate([out_heads, out_conv], axis=0)
    partial_sum = jnp.dot(mixer_rows, out_weight, preferred_element_type=jnp.float32)
    mixed = sum_groups(partial_sum.astype(jnp.bfloat16))
    return mixed[None]


def solution(mesh):
    in_specs = (
        P("fs", "sp", None),
        P(),
        P("fs", "tp"),
        P("fs", "tp"),
        P(),
        P("fs", "tp"),
        P("fs", "tp"),
        P("fs", "tp"),
        P(),
        P(),
        P(),
        P(),
        P("fs", "tp"),
        P("fs", "tp"),
        P(None, "tp"),
        P("tp"),
        P("tp"),
        P("tp", "fs"),
        P("tp", "fs"),
    )
    out_specs = P("fs", "sp", None)
    return jax.shard_map(local, mesh=mesh, in_specs=in_specs, out_specs=out_specs, check_vma=False)
```
